32 devices in a mesh: ep: 4 (over y, x), tp: 8 (over z, core).
Axes of the slice: x: 2, y: 2, z: 4, core: 2. Of those that a mesh axis runs over, the one named last changes fastest.
Arguments:
- queries: bfloat16 [16, 64, 2, 512], P('tp', None, None, 'ep'), may hold values from -24 to 24
- key_vectors: bfloat16 [16, 64, 2, 512], P('tp', None, None, 'ep'), may hold values from -24 to 24
- value_vectors: bfloat16 [16, 64, 2, 512], P('tp', None, None, 'ep'), may hold values from -6 to 6
- mixer_weight: bfloat16 [1024, 2048], replicated, may hold values from -0.375 to 0.375
- expert_rows: bfloat16 [512, 2048], P('ep'), may hold values from -6 to 6
- norm_gain: float32 [2048], replicated, may hold values from 0.1 to 1.9
- route_ids: int32 [512, 2], P('ep'), may hold values from 0 to 7, all different within a row; in each aligned block of 128 rows (0 to 127, 128 to 255, ...) at most 64 rows name the same one
- route_logits: float32 [512, 2], P('ep'), may hold values from -4 to 4
- gate_weight: bfloat16 [8, 2048, 4096], P('ep', None, 'tp'), may hold values from -0.39648438 to 0.39648438
- up_weight: bfloat16 [8, 2048, 4096], P('ep', None, 'tp'), may hold values from -0.39648438 to 0.39648438
- down_weight: bfloat16 [8, 4096, 2048], P('ep', 'tp'), may hold values from -0.028076172 to 0.028076172
Outputs:
- mixer_out: bfloat16 [2, 512, 2048], P(None, ('ep', 'tp'))
- routed_out: bfloat16 [2048, 512], P('tp', 'ep')
The draws below stay inside these ranges and needn't reach their ends.
Inputs may be any that keep to these rules, and one draw needn't show every extreme that they name: `route_ids`: each row names 2 different experts. Among the 128 rows of one index of ep no expert is named more than 64 times, a bound that some expert reaches in such a block.
All inputs are finite; a program needn't handle non-finite values.
Results may differ from the reference program's by a relative error of at most 0.018.
Values may be sent and summed in bfloat16 or wider, within the bound.
No kernel may reach another device: no remote copies, remote signals or barrier semaphores. Data moves between devices by JAX's collectives and lax.ppermute only.
A program may use at most 64 MiB of HBM per device.

```python
import math
import jax
import jax.numpy as jnp
import numpy as np
from jax import lax

D = 2048
HEADS = 16
HD = 64
FF = 4096
TOP = 2
SEQS = 2
SEG = 128
B_EP = 128
EXPERTS = 8
FF_DEV = 512
CAP = 64
LEN = 512
TOKENS_B = 512
N_EP = 4
N_TP = 8


def head_axes(key):
    direction = jax.random.normal(jax.random.fold_in(key, 101), (HEADS, HD), jnp.float32)
    return direction / jnp.sqrt(jnp.sum(direction * direction, axis=1, keepdims=True))


def noise_draw(key, array_shape):
    return jnp.clip(jax.random.normal(key, array_shape, jnp.float32), -4.0, 4.0)


def draw_queries(key, part):
    direction = head_axes(key)
    noise_part = noise_draw(jax.random.fold_in(key, 1), (HEADS, HD, SEQS, LEN))
    return (math.sqrt(HD) * direction[:, :, None, None] + noise_part).astype(jnp.bfloat16)


def draw_key_vectors(key, part):
    direction = head_axes(key)
    slow_rate = math.log(LEN) + 3.0
    fast_heads = jax.random.randint(jax.random.fold_in(key, 103), (HEADS,), 0, 2)
    reference_level = jnp.where(fast_heads > 0, 5.0, slow_rate).astype(jnp.float32)
    noise_perturbation = jax.random.uniform(jax.random.fold_in(key, 105), (HEADS, SEQS, LEN // SEG), jnp.float32, -0.7, 0.7)
    noise_perturbation = jnp.repeat(noise_perturbation, SEG, axis=2)
    element_locations = jax.random.randint(jax.random.fold_in(key, 107), (HEADS, SEQS, 3), 0, LEN)
    target_slot_numbers = jnp.arange(LEN, dtype=jnp.int32)
    spike_location = jnp.any(target_slot_numbers[None, None, :, None] == element_locations[:, :, None, :], axis=3)
    lookup_occurrence = jnp.where(spike_location, 0.5, reference_level[:, None, None] + noise_perturbation)
    noise_part = noise_draw(jax.random.fold_in(key, 2), (HEADS, HD, SEQS, LEN))
    return (noise_part - lookup_occurrence[:, None, :, :] * direction[:, :, None, None]).astype(jnp.bfloat16)


def raised(result, key, source, target, shards_of, factor):
    def block_of(dim):
        return (jnp.arange(result.shape[dim]) // (result.shape[dim] // shards_of)).reshape((-1,) + (1,) * (result.ndim - 1 - dim))

    one_side = jax.random.permutation(key, shards_of)[block_of(target)]
    second = (block_of(target) + shards_of // 2) % shards_of
    return jnp.where((block_of(source) == one_side) | (block_of(source) == second), factor * result, result)


def block_levels(stream_key, extent, cuts, smallest, top_value):
    level = 1.0
    for dim, blocks in cuts:
        draws = jax.random.uniform(jax.random.fold_in(jax.random.fold_in(stream_key, 6), dim), (blocks,), jnp.float32, smallest / len(cuts), top_value / len(cuts))
        level = level * jnp.repeat(jnp.exp(draws), extent[dim] // blocks).reshape((-1,) + (1,) * (len(extent) - 1 - dim))
    return level


def deal_out(own_key, own, number, rows, count, top, most, slope):
    order = jax.random.permutation(own_key, count)
    crowded, usual = portions_of(count, rows * top, most, slope, True), portions_of(count, rows * top, most, slope, False)
    places = jnp.arange(count)

    def named(sizes, rotation):
        used = int((sizes > 0).sum())
        fixed = max(1, used // 4)
        passed = fixed + (places - fixed + rotation * (used - fixed)) % max(1, count - fixed)
        return jnp.zeros((count,), jnp.int32).at[order[jnp.where(places < fixed, places, passed)]].set(jnp.asarray(sizes, jnp.int32))

    sizes = jnp.where(number % 4 == 0, named(crowded, number // 4), named(usual, number - number // 4 - 1))
    mixed = jax.random.permutation(jax.random.fold_in(own, 3), count)
    donor, taker = mixed[0:count // 2 * 2:2], mixed[1:count // 2 * 2:2]
    margin = jnp.minimum(sizes[donor] - 1, most - sizes[taker]) // 2
    margin = jnp.where((donor == order[0]) | (taker == order[0]) | (sizes[taker] == 0), 0, jnp.maximum(margin, 0))
    passed = jax.random.randint(jax.random.fold_in(own, 4), (count // 2,), 0, 1 << 20) % (margin + 1)
    sizes = sizes.at[donor].add(-passed).at[taker].add(passed)
    items = jnp.searchsorted(jnp.cumsum(sizes), jnp.arange(rows * top), side="right").astype(jnp.int32)
    table = items.reshape(top, rows).T
    table = table[jax.random.permutation(jax.random.fold_in(own, 1), rows)]
    rotation = jax.random.randint(jax.random.fold_in(own, 2), (rows, 1), 0, top)
    return jnp.take_along_axis(table, (jnp.arange(top)[None, :] + rotation) % top, axis=1)


def portions_of(number_of, total, most, slope, full):
    loads = [(1 << 20) // math.isqrt(grade ** slope) + 1 for grade in range(1, number_of + 1)]
    largest = most if full else min(most, max(-(-total // number_of), total * loads[0] // sum(loads)))
    least = 1 if total - largest >= number_of - 1 else 0
    given, rest = [largest] + [least] * (number_of - 1), total - largest - least * (number_of - 1)
    while rest > 0:
        movable = [i for i in range(1, number_of) if given[i] < largest] or [i for i in range(1, number_of) if given[i] < most]
        mass, left = sum([loads[i] for i in movable]), rest
        for i in movable:
            extra = min(most - given[i], max(1, left * loads[i] // mass), rest)
            given[i] = given[i] + extra
            rest = rest - extra
    return np.array(given)


def normal_values(key, extent, width, bound, split=(), held_as=jnp.bfloat16):
    result = jax.random.normal(key, extent, jnp.float32) * width
    if len(split) > 0:
        result = block_levels(key, extent, split, -0.22, 0.18) * result
    return jnp.clip(result, min=-bound, max=bound).astype(held_as)


def noise_with(stream_key, extent, width, most, cuts, heavy, kind=jnp.bfloat16):
    values = width * jax.random.normal(stream_key, extent, jnp.float32)
    if cuts:
        values = values * block_levels(stream_key, extent, cuts, -0.22, 0.18)
    return jnp.clip(raised(values, jax.random.fold_in(stream_key, 3), *heavy), -most, most).astype(kind)


def setup_inputs(seed: int = 0) -> dict:
    key_of = jax.random.split(jax.random.key(seed), 12)
    queries = draw_queries(jax.random.fold_in(key_of[11], 71), 0)
    key_vectors = draw_key_vectors(jax.random.fold_in(key_of[11], 71), 0)
    value_vectors = normal_values(key_of[2], (HEADS, HD, SEQS, LEN), 1.0, 6.0, ((0, 8), (3, 4)))
    mixer_weight = normal_values(key_of[3], (HEADS * HD, D), (HEADS * HD // 4) ** -0.5, 0.375)
    expert_rows = normal_values(key_of[4], (TOKENS_B, D), 1.0, 6.0, ((0, 4),))
    norm_gain = jnp.clip(1.0 + 0.18 * jax.random.normal(key_of[5], (D,), jnp.float32), 0.1, 1.9)
    route_ids_keys = jax.random.split(jax.random.fold_in(key_of[6], 1), TOKENS_B // B_EP)
    route_ids_turns = jax.random.permutation(jax.random.fold_in(key_of[6], 3), TOKENS_B // B_EP)
    route_ids = jax.vmap(lambda own, number: deal_out(jax.random.fold_in(key_of[6], 2), own, number, B_EP, EXPERTS, TOP, CAP, 2))(route_ids_keys, route_ids_turns).reshape((TOKENS_B, TOP))
    route_logits = normal_values(key_of[7], (TOKENS_B, TOP), 1.0, 4.0, ((0, 4),), jnp.float32)
    gate_weight = normal_values(key_of[8], (EXPERTS, D, FF), (3.0 * D ** -0.5), 0.39648438, ((0, 4), (2, 8)))
    up_weight = normal_values(key_of[9], (EXPERTS, D, FF), (3.0 * D ** -0.5), 0.39648438, ((0, 4), (2, 8)))
    down_weight = noise_with(key_of[10], (EXPERTS, FF, D), (0.3 * FF ** -0.5), 0.028076172, ((0, 4), (1, 8)), (1, 2, 8, 2.0))
    return {"queries": queries, "key_vectors": key_vectors, "value_vectors": value_vectors, "mixer_weight": mixer_weight, "expert_rows": expert_rows, "norm_gain": norm_gain, "route_ids": route_ids, "route_logits": route_logits, "gate_weight": gate_weight, "up_weight": up_weight, "down_weight": down_weight}


limit_value = 7.0
alpha_value = 1.702
norm_eps = 1e-06

def activate(gate_pre, up_pre):
    gate_clamped = jnp.minimum(gate_pre, limit_value)
    up_clamped = jnp.clip(up_pre, -limit_value, limit_value)
    return ((up_clamped + 1.0) * gate_clamped * jax.nn.sigmoid(alpha_value * gate_clamped)).astype(jnp.bfloat16)

def stick_block(query_part, key_part, value_part, query_start):
    scores = jnp.einsum('hdq,hdk->hqk', query_part.astype(jnp.float32), key_part.astype(jnp.float32)) * HD ** (-0.5)
    query_pos = query_start + lax.broadcasted_iota(jnp.int32, (SEG, LEN), 0)
    lookup_slot = lax.broadcasted_iota(jnp.int32, (SEG, LEN), 1)
    usable = (lookup_slot < query_pos)[None]
    log_keep = jnp.where(usable, jax.nn.log_sigmoid(-scores), 0.0)
    blocked = log_keep.reshape(HEADS, SEG, N_EP, SEG)
    within = lax.cumsum(blocked, axis=3, reverse=True) - blocked
    block_totals = lax.optimization_barrier(jnp.sum(blocked, axis=3))
    log_beta = jax.nn.log_sigmoid(scores).reshape(HEADS, SEG, N_EP, SEG)
    weight = jnp.where(usable.reshape(1, SEG, N_EP, SEG), jnp.exp(log_beta + within), 0.0).astype(jnp.bfloat16)
    block_values = jnp.einsum('hqbk,hdbk->hdqb', weight.astype(jnp.float32), value_part.reshape(HEADS, HD, N_EP, SEG).astype(jnp.float32))
    later_sums = lax.cumsum(block_totals, axis=2, reverse=True) - block_totals
    return lax.optimization_barrier(jnp.sum(jnp.exp(later_sums)[:, None] * block_values, axis=3)).astype(jnp.bfloat16)

def reference(queries, key_vectors, value_vectors, mixer_weight, expert_rows, norm_gain, route_ids, route_logits, gate_weight, up_weight, down_weight):

    def one_block(block_number):
        seq_index = block_number // N_EP
        query_start = (block_number % N_EP * SEG).astype(jnp.int32)
        query_seq = lax.dynamic_index_in_dim(queries, seq_index, 2, keepdims=False)
        query_part = lax.dynamic_slice_in_dim(query_seq, query_start, SEG, 2)
        key_part = lax.dynamic_index_in_dim(key_vectors, seq_index, 2, keepdims=False)
        value_part = lax.dynamic_index_in_dim(value_vectors, seq_index, 2, keepdims=False)
        return stick_block(query_part, key_part, value_part, query_start)
    attended = lax.map(one_block, jnp.arange(SEQS * N_EP, dtype=jnp.int32))
    attended = attended.reshape(SEQS, N_EP, HEADS, HD, SEG).transpose(0, 1, 4, 2, 3).reshape(SEQS, LEN, HEADS * HD)
    mixer_out = jnp.einsum('slc,cm->slm', attended.astype(jnp.float32), mixer_weight.astype(jnp.float32)).astype(jnp.bfloat16)
    values = expert_rows.astype(jnp.float32)
    scaled = values * lax.rsqrt(lax.optimization_barrier(jnp.mean(values * values, axis=-1, keepdims=True)) + norm_eps)
    normed = (scaled * norm_gain).astype(jnp.bfloat16)
    route_weight = jax.nn.softmax(route_logits, axis=-1)
    block_ids = route_ids.reshape(N_EP, B_EP * TOP)
    one_hot_matrix = (block_ids[:, :, None] == jnp.arange(EXPERTS, dtype=jnp.int32)[None, None, :]).astype(jnp.int32)
    earlier = jnp.cumsum(one_hot_matrix, axis=1) - one_hot_matrix
    slot_rank = lax.optimization_barrier(jnp.sum(earlier * one_hot_matrix, axis=2))
    source = jnp.arange(N_EP, dtype=jnp.int32)[:, None]
    token_index = source * B_EP + jnp.arange(B_EP * TOP, dtype=jnp.int32)[None, :] // TOP
    table_index = ((block_ids * N_EP + source) * CAP + slot_rank).reshape(-1).astype(jnp.int32)
    owner_token = jnp.zeros((EXPERTS * N_EP * CAP,), jnp.int32).at[table_index].set(token_index.reshape(-1))
    slot_rows = N_EP * CAP

    def one_expert(expert_index):
        owners = lax.dynamic_slice_in_dim(owner_token, expert_index * slot_rows, slot_rows)
        rows_in = normed[owners]
        gate_pre = jnp.dot(rows_in, lax.dynamic_index_in_dim(gate_weight, expert_index, 0, keepdims=False), preferred_element_type=jnp.float32)
        up_pre = jnp.dot(rows_in, lax.dynamic_index_in_dim(up_weight, expert_index, 0, keepdims=False), preferred_element_type=jnp.float32)
        hidden = activate(gate_pre, up_pre)
        down_part = lax.dynamic_index_in_dim(down_weight, expert_index, 0, keepdims=False)
        group_part = jnp.einsum('rgf,gfd->grd', hidden.reshape(slot_rows, N_TP, FF_DEV).astype(jnp.float32), down_part.reshape(N_TP, FF_DEV, D).astype(jnp.float32))
        rounded = lax.optimization_barrier(group_part.astype(jnp.bfloat16))
        return lax.optimization_barrier(jnp.sum(rounded.astype(jnp.float32), axis=0))
    expert_value = lax.map(one_expert, jnp.arange(EXPERTS, dtype=jnp.int32)).reshape(EXPERTS * slot_rows, D)
    picked = expert_value[table_index].reshape(TOKENS_B, TOP, D)
    combined = lax.optimization_barrier(jnp.sum(picked * route_weight[:, :, None], axis=1))
    routed_out = combined.T.astype(jnp.bfloat16)
    return (mixer_out, routed_out)
```

```python
import functools

import jax
import jax.numpy as jnp
from jax import lax
from jax.experimental import pallas as pl
from jax.experimental.pallas import tpu as pltpu
from jax.sharding import PartitionSpec as P

limit_value = 7.0
alpha_value = 1.702
norm_eps = 1e-06
LANES = 128


def swap(x, axis, distance):
    n = lax.axis_size(axis)
    return lax.ppermute(x, axis, [(i, i ^ distance) for i in range(n)])


def dot_f32(a, b, dims):
    return lax.dot_general(a, b, (dims, ((), ())), preferred_element_type=jnp.float32)


def prep_kernel(core_ref, rows_ref, gain_ref, ids_ref, logits_ref, full_ref, half_ref, *, experts):
    width = rows_ref.shape[1]
    values = rows_ref[...].astype(jnp.float32)
    mean = jnp.mean(values * values, axis=-1, keepdims=True)
    normed = (values * lax.rsqrt(mean + norm_eps) * gain_ref[...]).astype(jnp.bfloat16)
    full_ref[:, :width] = normed
    ids = ids_ref[...]
    logits = logits_ref[...]
    top = jnp.max(logits, axis=-1, keepdims=True)
    powers = jnp.exp(logits - top)
    weights = powers / jnp.sum(powers, axis=-1, keepdims=True)
    lane = lax.broadcasted_iota(jnp.int32, (ids.shape[0], LANES), 1)
    low_lane = lane - experts
    high = jnp.zeros(lane.shape, jnp.float32)
    low = jnp.zeros(lane.shape, jnp.float32)
    for k in range(ids.shape[1]):
        w = weights[:, k : k + 1]
        w_high = w.astype(jnp.bfloat16).astype(jnp.float32)
        high = high + jnp.where(lane == ids[:, k : k + 1], w_high, 0.0)
        low = low + jnp.where(low_lane == ids[:, k : k + 1], w - w_high, 0.0)
    full_ref[:, width:] = (high + low).astype(jnp.bfloat16)
    half = half_ref.shape[0]
    half_ref[...] = full_ref[pl.ds(pl.multiple_of(core_ref[0] * half, half), half), :]


def prepare(core, expert_rows, norm_gain, route_ids, route_logits, experts):
    rows, width = expert_rows.shape
    vmem = pl.BlockSpec(memory_space=pltpu.VMEM)
    return pl.pallas_call(
        functools.partial(prep_kernel, experts=experts),
        out_shape=(
            jax.ShapeDtypeStruct((rows, width + LANES), jnp.bfloat16),
            jax.ShapeDtypeStruct((rows // 2, width + LANES), jnp.bfloat16),
        ),
        in_specs=[pl.BlockSpec(memory_space=pltpu.SMEM), vmem, vmem, vmem, vmem],
        out_specs=(vmem, vmem),
        name="prep",
    )(core, expert_rows, norm_gain.reshape(1, width), route_ids, route_logits)


def expert_kernel(place_ref, *refs, parts, experts, local, steps, chunks):
    own_ref, mine_in, other_in = refs[0], refs[1:parts], refs[parts : 2 * parts - 1]
    gate_ref, up_ref, down_ref = refs[2 * parts - 1 : 2 * parts + 2]
    outs = refs[2 * parts + 2 : 4 * parts + 2]
    mine_out, other_out = outs[:parts], outs[parts:]
    rows_ref, weight_ref, hidden_ref = refs[4 * parts + 2 :]
    step = pl.program_id(0)
    rows = own_ref.shape[0]
    half = rows // 2
    width = rows_ref.shape[1]
    core = place_ref[1]

    @pl.when(step == 0)
    def _():
        rows_ref[:rows, :] = own_ref[:, :width]
        weight_ref[:rows, :] = own_ref[:, width:].astype(jnp.float32)
        for d in range(1, parts):
            for ref, side in ((mine_in[d - 1], core), (other_in[d - 1], 1 - core)):
                at = pl.ds(pl.multiple_of(d * rows + side * half, half), half)
                rows_ref[at, :] = ref[:, :width]
                weight_ref[at, :] = ref[:, width:].astype(jnp.float32)

    @pl.when(step < steps)
    def _():
        x = rows_ref[...]
        gate = dot_f32(x, gate_ref[0], ((1,), (0,)))
        up = dot_f32(x, up_ref[0], ((1,), (0,)))
        expert = place_ref[0] * local + step // chunks
        table = weight_ref[...]
        lane = lax.broadcasted_iota(jnp.int32, table.shape, 1)
        chosen = jnp.logical_or(lane == expert, lane == expert + experts)
        weight = jnp.sum(jnp.where(chosen, table, 0.0), axis=1, keepdims=True)
        gate = jnp.minimum(gate, limit_value)
        up = jnp.clip(up, -limit_value, limit_value)
        hidden = (up + 1.0) * gate / (1.0 + jnp.exp(-alpha_value * gate)) * weight
        hidden_ref[step] = hidden.astype(jnp.bfloat16)

    @pl.when(step >= steps)
    def _():
        chunk = hidden_ref.shape[2]
        total = dot_f32(hidden_ref[0], down_ref[:chunk, :], ((1,), (0,)))
        for p in range(1, steps):
            total = total + dot_f32(
                hidden_ref[p], down_ref[p * chunk : (p + 1) * chunk, :], ((1,), (0,))
            )
        slice_width = total.shape[1] // 2
        first = total[:, :slice_width]
        second = total[:, slice_width:]
        mine = jnp.where(core == 0, first, second).astype(jnp.bfloat16)
        other = jnp.where(core == 0, second, first).astype(jnp.bfloat16)
        for d in range(parts):
            mine_out[d][...] = mine[d * rows : (d + 1) * rows, :]
            other_out[d][...] = other[d * rows : (d + 1) * rows, :]


def run_experts(place, own, mine_in, other_in, gate_weight, up_weight, down_weight, experts, tp):
    parts = 1 + len(mine_in)
    rows = own.shape[0]
    local, width, units = gate_weight.shape
    chunk = min(256, units)
    chunks = units // chunk
    steps = local * chunks
    slice_width = width // tp
    columns = tp // 2

    def whole(x):
        return pl.BlockSpec(x.shape, lambda i: (0, 0))

    def weight_map(i):
        j = jnp.minimum(i, steps - 1)
        return (j // chunks, 0, j % chunks)

    def column_map(i):
        return (0, jnp.maximum(i - steps, 0))

    weight_spec = pl.BlockSpec((1, width, chunk), weight_map)
    out_spec = pl.BlockSpec((rows, slice_width), column_map)
    outs = pl.pallas_call(
        functools.partial(
            expert_kernel, parts=parts, experts=experts, local=local, steps=steps, chunks=chunks
        ),
        grid=(steps + columns,),
        out_shape=[jax.ShapeDtypeStruct((rows, width // 2), jnp.bfloat16)] * (2 * parts),
        in_specs=[pl.BlockSpec(memory_space=pltpu.SMEM)]
        + [whole(x) for x in (own, *mine_in, *other_in)]
        + [
            weight_spec,
            weight_spec,
            pl.BlockSpec((local * units, 2 * slice_width), column_map),
        ],
        out_specs=[out_spec] * (2 * parts),
        scratch_shapes=[
            pltpu.VMEM((parts * rows, width), jnp.bfloat16),
            pltpu.VMEM((parts * rows, LANES), jnp.float32),
            pltpu.VMEM((steps, parts * rows, chunk), jnp.bfloat16),
        ],
        compiler_params=pltpu.CompilerParams(dimension_semantics=("arbitrary",)),
        name="experts",
    )(
        place, own, *mine_in, *other_in, gate_weight, up_weight,
        down_weight.reshape(local * units, width),
    )
    return outs[:parts], outs[parts:]


def route_experts(
    expert_rows, norm_gain, route_ids, route_logits, gate_weight, up_weight, down_weight
):
    groups = lax.axis_size("ep")
    tp = lax.axis_size("tp")
    tp_index = lax.axis_index("tp")
    core = tp_index % 2
    experts = groups * gate_weight.shape[0]
    slice_width = expert_rows.shape[1] // tp
    place = jnp.stack([lax.axis_index("ep"), core]).astype(jnp.int32)
    own, half = prepare(place[1:], expert_rows, norm_gain, route_ids, route_logits, experts)
    mine_in = [swap(half, "ep", d) for d in range(1, groups)]
    other_in = [swap(x, "tp", 1) for x in mine_in]
    mine, other = run_experts(
        place, own, mine_in, other_in, gate_weight, up_weight, down_weight, experts, tp
    )
    pair = [
        m.astype(jnp.float32) + swap(o, "tp", 1).astype(jnp.float32) for m, o in zip(mine, other)
    ]
    total = pair[0]
    for d in range(1, groups):
        total = total + swap(pair[d].astype(jnp.bfloat16), "ep", d).astype(jnp.float32)
    plane = tp_index // 2

    def columns_of(k):
        return lax.dynamic_slice_in_dim(total, (plane ^ k) * slice_width, slice_width, 1)

    result = columns_of(0)
    for k in range(1, tp // 2):
        result = result + swap(columns_of(k).astype(jnp.bfloat16), "tp", 2 * k).astype(jnp.float32)
    return result.T.astype(jnp.bfloat16)


def attend_kernel(own_ref, query_ref, *refs):
    blocks, out_ref = refs[:-1], refs[-1]
    heads, seqs, head_dim, seg = query_ref.shape
    own = own_ref[0]
    pairs = [(s, h) for s in range(seqs) for h in range(heads)]
    rows = len(pairs) * seg
    scale = head_dim ** (-0.5)
    query_pos = lax.broadcasted_iota(jnp.int32, (rows, seg), 0) % seg
    slot = lax.broadcasted_iota(jnp.int32, (rows, seg), 1)
    j = lax.broadcasted_iota(jnp.int32, (seg, 2 * seg), 0)
    u = lax.broadcasted_iota(jnp.int32, (seg, 2 * seg), 1)
    sums = jnp.where(jnp.logical_or(j > u, u >= seg), 1.0, 0.0).astype(jnp.bfloat16)
    values, totals = [], []
    for d, block in enumerate(blocks):
        index = own ^ d
        scores = scale * jnp.concatenate(
            [dot_f32(query_ref[h, s], block[0, h, s], ((0,), (0,))) for s, h in pairs], axis=0
        )
        usable = slot < query_pos + (own - index) * seg
        tail = jnp.log1p(jnp.exp(-jnp.abs(scores)))
        keep = jnp.where(usable, -jnp.maximum(scores, 0.0) - tail, 0.0)
        high = keep.astype(jnp.bfloat16)
        low = (keep - high.astype(jnp.float32)).astype(jnp.bfloat16)
        both = dot_f32(high, sums, ((1,), (0,))) + dot_f32(low, sums, ((1,), (0,)))
        weight = jnp.where(
            usable, jnp.exp(jnp.minimum(scores, 0.0) - tail + both[:, :seg]), 0.0
        ).astype(jnp.bfloat16)
        totals.append(both[:, seg : seg + head_dim])
        values.append(
            jnp.concatenate(
                [
                    dot_f32(weight[i * seg : (i + 1) * seg], block[1, h, s], ((1,), (1,)))
                    for i, (s, h) in enumerate(pairs)
                ],
                axis=0,
            )
        )
    out = jnp.zeros(values[0].shape, jnp.float32)
    for d in range(len(blocks)):
        later = jnp.zeros(values[0].shape, jnp.float32)
        for f in range(len(blocks)):
            if f != d:
                later = later + jnp.where((own ^ f) > (own ^ d), totals[f], 0.0)
        out = out + jnp.exp(later) * values[d]
    out_ref[...] = jnp.concatenate(
        [out[i * seg : (i + 1) * seg] for i in range(len(pairs))], axis=1
    ).astype(jnp.bfloat16)


def attend(queries, key_vectors, value_vectors):
    heads, head_dim, seqs, seg = queries.shape
    blocks = lax.axis_size("ep")
    own_index = lax.axis_index("ep").astype(jnp.int32).reshape(1)
    query_rows = queries.transpose(0, 2, 1, 3)
    own = jnp.stack([key_vectors, value_vectors]).transpose(0, 1, 3, 2, 4)
    gathered = [own] + [swap(own, "ep", d) for d in range(1, blocks)]
    vmem = pl.BlockSpec(memory_space=pltpu.VMEM)
    return pl.pallas_call(
        attend_kernel,
        out_shape=jax.ShapeDtypeStruct((seg, seqs * heads * head_dim), jnp.bfloat16),
        in_specs=[pl.BlockSpec(memory_space=pltpu.SMEM)] + [vmem] * (blocks + 1),
        out_specs=vmem,
        name="attend",
    )(own_index, query_rows, *gathered)


def mix_heads(attended, mixer_weight, seqs):
    tp = lax.axis_size("tp")
    seg, columns = attended.shape
    channels = columns // seqs
    pieces = lax.all_to_all(
        attended.reshape(tp, seg // tp, columns), "tp", split_axis=0, concat_axis=0, tiled=True
    ).reshape(tp, seg // tp, seqs, channels)
    rows = pieces.transpose(2, 1, 0, 3).reshape(seqs * (seg // tp), tp * channels)
    out = dot_f32(rows, mixer_weight, ((1,), (0,))).astype(jnp.bfloat16)
    return out.reshape(seqs, seg // tp, mixer_weight.shape[1])


def body(
    queries,
    key_vectors,
    value_vectors,
    mixer_weight,
    expert_rows,
    norm_gain,
    route_ids,
    route_logits,
    gate_weight,
    up_weight,
    down_weight,
):
    attended = attend(queries, key_vectors, value_vectors)
    mixer_out = mix_heads(attended, mixer_weight, queries.shape[2])
    routed_out = route_experts(
        expert_rows, norm_gain, route_ids, route_logits, gate_weight, up_weight, down_weight
    )
    return (mixer_out, routed_out)


def solution(mesh):
    in_specs = (
        P("tp", None, None, "ep"),
        P("tp", None, None, "ep"),
        P("tp", None, None, "ep"),
        P(),
        P("ep", None),
        P(),
        P("ep", None),
        P("ep", None),
        P("ep", None, "tp"),
        P("ep", None, "tp"),
        P("ep", "tp", None),
    )
    out_specs = (P(None, ("ep", "tp"), None), P("tp", "ep"))
    return jax.shard_map(body, mesh=mesh, in_specs=in_specs, out_specs=out_specs, check_vma=False)
```

```python
import functools

import jax
import jax.numpy as jnp
from jax import lax
from jax.experimental import pallas as pl
from jax.experimental.pallas import tpu as pltpu
from jax.sharding import PartitionSpec as P


limit_value = 7.0
alpha_value = 1.702
norm_eps = 1e-06
LANES = 128


def swap(x, axis, distance):
    n = lax.axis_size(axis)
    return lax.ppermute(x, axis, [(i, i ^ distance) for i in range(n)])


def dot_f32(a, b, dims):
    return lax.dot_general(a, b, (dims, ((), ())), preferred_element_type=jnp.float32)


def prep_kernel(core_ref, rows_ref, gain_ref, ids_ref, logits_ref, full_ref, half_ref, *, experts):
    width = rows_ref.shape[1]
    values = rows_ref[...].astype(jnp.float32)
    mean = jnp.mean(values * values, axis=-1, keepdims=True)
    normed = (values * lax.rsqrt(mean + norm_eps) * gain_ref[...]).astype(jnp.bfloat16)
    full_ref[:, :width] = normed
    ids = ids_ref[...]
    logits = logits_ref[...]
    top = jnp.max(logits, axis=0, keepdims=True)
    powers = jnp.exp(logits - top)
    weights = powers / jnp.sum(powers, axis=0, keepdims=True)
    line = lax.broadcasted_iota(jnp.int32, (LANES, ids.shape[1]), 0)
    low_line = line - experts
    table = jnp.zeros(line.shape, jnp.float32)
    for k in range(ids.shape[0]):
        w = weights[k : k + 1]
        w_high = w.astype(jnp.bfloat16).astype(jnp.float32)
        table = table + jnp.where(line == ids[k : k + 1], w_high, 0.0)
        table = table + jnp.where(low_line == ids[k : k + 1], w - w_high, 0.0)
    full_ref[:, width:] = table.T.astype(jnp.bfloat16)
    half = half_ref.shape[0]
    half_ref[...] = full_ref[pl.ds(pl.multiple_of(core_ref[0] * half, half), half), :]


def prepare(core, expert_rows, norm_gain, route_ids, route_logits, experts):
    rows, width = expert_rows.shape
    vmem = pl.BlockSpec(memory_space=pltpu.VMEM)
    return pl.pallas_call(
        functools.partial(prep_kernel, experts=experts),
        out_shape=(
            jax.ShapeDtypeStruct((rows, width + LANES), jnp.bfloat16),
            jax.ShapeDtypeStruct((rows // 2, width + LANES), jnp.bfloat16),
        ),
        in_specs=[pl.BlockSpec(memory_space=pltpu.SMEM), vmem, vmem, vmem, vmem],
        out_specs=(vmem, vmem),
        name="prep",
    )(core, expert_rows, norm_gain.reshape(1, width), route_ids.T, route_logits.T)


def expert_kernel(place_ref, *refs, whole, pairs, experts, local, steps, chunks):
    parts = whole + pairs
    inputs, refs = refs[: whole + 2 * pairs], refs[whole + 2 * pairs :]
    gate_ref, up_ref, down_ref = refs[:3]
    mine_out, other_out = refs[3 : 3 + parts], refs[3 + parts : 3 + 2 * parts]
    rows_ref, weight_ref, hidden_ref = refs[3 + 2 * parts :]
    step = pl.program_id(0)
    rows = mine_out[0].shape[0]
    half = rows // 2
    width = rows_ref.shape[1]
    core = place_ref[1]

    @pl.when(step == 0)
    def _():
        for d in range(whole):
            at = slice(d * rows, (d + 1) * rows)
            rows_ref[at, :] = inputs[d][:, :width]
            weight_ref[at, :] = inputs[d][:, width:].astype(jnp.float32)
        for d in range(pairs):
            for ref, side in (
                (inputs[whole + d], core),
                (inputs[whole + pairs + d], 1 - core),
            ):
                start = (whole + d) * rows + side * half
                at = pl.ds(pl.multiple_of(start, half), half)
                rows_ref[at, :] = ref[:, :width]
                weight_ref[at, :] = ref[:, width:].astype(jnp.float32)

    @pl.when(step < steps)
    def _():
        x = rows_ref[...]
        gate = dot_f32(x, gate_ref[0], ((1,), (0,)))
        up = dot_f32(x, up_ref[0], ((1,), (0,)))
        expert = place_ref[0] * local + step // chunks
        table = weight_ref[...]
        lane = lax.broadcasted_iota(jnp.int32, table.shape, 1)
        chosen = jnp.logical_or(lane == expert, lane == expert + experts)
        weight = jnp.sum(jnp.where(chosen, table, 0.0), axis=1, keepdims=True)
        gate = jnp.minimum(gate, limit_value)
        up = jnp.clip(up, -limit_value, limit_value)
        hidden = (up + 1.0) * gate / (1.0 + jnp.exp(-alpha_value * gate)) * weight
        hidden_ref[step] = hidden.astype(jnp.bfloat16)

    @pl.when(step >= steps)
    def _():
        chunk = hidden_ref.shape[2]
        total = dot_f32(hidden_ref[0], down_ref[:chunk, :], ((1,), (0,)))
        for p in range(1, steps):
            total = total + dot_f32(
                hidden_ref[p], down_ref[p * chunk : (p + 1) * chunk, :], ((1,), (0,))
            )
        slice_width = total.shape[1] // 2
        first = total[:, :slice_width]
        second = total[:, slice_width:]
        mine = jnp.where(core == 0, first, second).astype(jnp.bfloat16)
        other = jnp.where(core == 0, second, first).astype(jnp.bfloat16)
        for d in range(parts):
            mine_out[d][...] = mine[d * rows : (d + 1) * rows, :]
            other_out[d][...] = other[d * rows : (d + 1) * rows, :]


def run_experts(place, own, mine_in, other_in, gate_weight, up_weight, down_weight, experts, tp):
    parts = len(own) + len(mine_in)
    rows = 2 * mine_in[0].shape[0]
    local, width, units = gate_weight.shape
    chunk = min(256, units)
    chunks = units // chunk
    steps = local * chunks
    slice_width = width // tp
    columns = tp // 2

    def whole(x):
        return pl.BlockSpec(x.shape, lambda i: (0, 0))

    def weight_map(i):
        j = jnp.minimum(i, steps - 1)
        return (j // chunks, 0, j % chunks)

    def column_map(i):
        return (0, jnp.maximum(i - steps, 0))

    weight_spec = pl.BlockSpec((1, width, chunk), weight_map)
    out_spec = pl.BlockSpec((rows, slice_width), column_map)
    outs = pl.pallas_call(
        functools.partial(
            expert_kernel,
            whole=len(own),
            pairs=len(mine_in),
            experts=experts,
            local=local,
            steps=steps,
            chunks=chunks,
        ),
        grid=(steps + columns,),
        out_shape=[jax.ShapeDtypeStruct((rows, width // 2), jnp.bfloat16)] * (2 * parts),
        in_specs=[pl.BlockSpec(memory_space=pltpu.SMEM)]
        + [whole(x) for x in (*own, *mine_in, *other_in)]
        + [
            weight_spec,
            weight_spec,
            pl.BlockSpec((local * units, 2 * slice_width), column_map),
        ],
        out_specs=[out_spec] * (2 * parts),
        scratch_shapes=[
            pltpu.VMEM((parts * rows, width), jnp.bfloat16),
            pltpu.VMEM((parts * rows, LANES), jnp.float32),
            pltpu.VMEM((steps, parts * rows, chunk), jnp.bfloat16),
        ],
        compiler_params=pltpu.CompilerParams(dimension_semantics=("arbitrary",)),
        name="experts",
    )(
        place, *own, *mine_in, *other_in, gate_weight, up_weight,
        down_weight.reshape(local * units, width),
    )
    return outs[:parts], outs[parts:]


def route_experts(own, half, place, attended, gate_weight, up_weight, down_weight):
    groups = lax.axis_size("ep")
    tp = lax.axis_size("tp")
    tp_index = lax.axis_index("tp")
    experts = groups * gate_weight.shape[0]
    slice_width = down_weight.shape[2] // tp
    order = sorted(range(1, groups), key=lambda d: -d.bit_count())
    early, late = order[: groups // 2 - 1], order[groups // 2 - 1 :]
    mine_in = {d: swap(half, "ep", d) for d in order}
    other_in = {d: swap(mine_in[d], "tp", 1) for d in order}
    weights = (gate_weight, up_weight, down_weight, experts, tp)

    def pair_sums(mine, other):
        return [
            m.astype(jnp.float32) + swap(o, "tp", 1).astype(jnp.float32)
            for m, o in zip(mine, other)
        ]

    own, attended = lax.optimization_barrier((own, attended))
    mine, other = run_experts(
        place, [own], [mine_in[d] for d in early], [other_in[d] for d in early], *weights
    )
    total, *sums = pair_sums(mine, other)
    first_sends = [x.astype(jnp.bfloat16) for x in sums]
    place, first_sends = lax.optimization_barrier((place, first_sends))
    returned = [swap(x, "ep", d) for d, x in zip(early, first_sends)]
    mine, other = run_experts(
        place, [], [mine_in[d] for d in late], [other_in[d] for d in late], *weights
    )
    attended, mine = lax.optimization_barrier((attended, mine))
    pieces = exchange_heads(attended)
    sends = [x.astype(jnp.bfloat16) for x in pair_sums(mine, other)]
    returned = returned + [swap(x, "ep", d) for d, x in zip(late, sends)]
    for x in returned:
        total = total + x.astype(jnp.float32)
    plane = tp_index // 2

    def columns_of(k):
        return lax.dynamic_slice_in_dim(total, (plane ^ k) * slice_width, slice_width, 1)

    result = columns_of(0)
    for k in range(1, tp // 2):
        result = result + swap(columns_of(k).astype(jnp.bfloat16), "tp", 2 * k).astype(jnp.float32)
    return result.T.astype(jnp.bfloat16), pieces


def attend_kernel(own_ref, query_ref, *refs):
    blocks, out_ref = refs[:-1], refs[-1]
    heads, seqs, head_dim, seg = query_ref.shape
    own = own_ref[0]
    pairs = [(s, h) for s in range(seqs) for h in range(heads)]
    rows = len(pairs) * seg
    scale = head_dim ** (-0.5)
    query_pos = lax.broadcasted_iota(jnp.int32, (rows, seg), 0) % seg
    slot = lax.broadcasted_iota(jnp.int32, (rows, seg), 1)
    j = lax.broadcasted_iota(jnp.int32, (seg, 2 * seg), 0)
    u = lax.broadcasted_iota(jnp.int32, (seg, 2 * seg), 1)
    sums = jnp.where(jnp.logical_or(j > u, u >= seg), 1.0, 0.0).astype(jnp.bfloat16)
    values, totals = [], []
    for d, block in enumerate(blocks):
        index = own ^ d
        scores = scale * jnp.concatenate(
            [dot_f32(query_ref[h, s], block[0, h, s], ((0,), (0,))) for s, h in pairs], axis=0
        )
        usable = slot < query_pos + (own - index) * seg
        tail = jnp.log1p(jnp.exp(-jnp.abs(scores)))
        keep = jnp.where(usable, -jnp.maximum(scores, 0.0) - tail, 0.0)
        high = keep.astype(jnp.bfloat16)
        low = (keep - high.astype(jnp.float32)).astype(jnp.bfloat16)
        both = dot_f32(high, sums, ((1,), (0,))) + dot_f32(low, sums, ((1,), (0,)))
        weight = jnp.where(
            usable, jnp.exp(jnp.minimum(scores, 0.0) - tail + both[:, :seg]), 0.0
        ).astype(jnp.bfloat16)
        totals.append(both[:, seg : seg + head_dim])
        values.append(
            jnp.concatenate(
                [
                    dot_f32(weight[i * seg : (i + 1) * seg], block[1, h, s], ((1,), (1,)))
                    for i, (s, h) in enumerate(pairs)
                ],
                axis=0,
            )
        )
    out = jnp.zeros(values[0].shape, jnp.float32)
    for d in range(len(blocks)):
        later = jnp.zeros(values[0].shape, jnp.float32)
        for f in range(len(blocks)):
            if f != d:
                later = later + jnp.where((own ^ f) > (own ^ d), totals[f], 0.0)
        out = out + jnp.exp(later) * values[d]
    out_ref[...] = jnp.concatenate(
        [out[i * seg : (i + 1) * seg] for i in range(len(pairs))], axis=1
    ).astype(jnp.bfloat16)


def gather_keys(own):
    return [own] + [swap(own, "ep", d) for d in range(1, lax.axis_size("ep"))]


def attend(query_rows, gathered):
    heads, seqs, head_dim, seg = query_rows.shape
    blocks = len(gathered)
    own_index = lax.axis_index("ep").astype(jnp.int32).reshape(1)
    vmem = pl.BlockSpec(memory_space=pltpu.VMEM)
    return pl.pallas_call(
        attend_kernel,
        out_shape=jax.ShapeDtypeStruct((seg, seqs * heads * head_dim), jnp.bfloat16),
        in_specs=[pl.BlockSpec(memory_space=pltpu.SMEM)] + [vmem] * (blocks + 1),
        out_specs=vmem,
        name="attend",
    )(own_index, query_rows, *gathered)


def exchange_heads(attended):
    tp = lax.axis_size("tp")
    seg, columns = attended.shape
    return lax.all_to_all(
        attended.reshape(tp, seg // tp, columns), "tp", split_axis=0, concat_axis=0, tiled=True
    )


def mix_heads(pieces, mixer_weight, seqs):
    tp, rows, columns = pieces.shape
    channels = columns // seqs
    pieces = pieces.reshape(tp, rows, seqs, channels)
    stacked = pieces.transpose(2, 1, 0, 3).reshape(seqs * rows, tp * channels)
    out = dot_f32(stacked, mixer_weight, ((1,), (0,))).astype(jnp.bfloat16)
    return out.reshape(seqs, rows, mixer_weight.shape[1])


def body(
    queries,
    key_vectors,
    value_vectors,
    mixer_weight,
    expert_rows,
    norm_gain,
    route_ids,
    route_logits,
    gate_weight,
    up_weight,
    down_weight,
):
    experts = lax.axis_size("ep") * gate_weight.shape[0]
    place = jnp.stack([lax.axis_index("ep"), lax.axis_index("tp") % 2]).astype(jnp.int32)
    keys = jnp.stack([key_vectors, value_vectors]).transpose(0, 1, 3, 2, 4)
    query_rows = queries.transpose(0, 2, 1, 3)
    keys, expert_rows = lax.optimization_barrier((keys, expert_rows))
    gathered = gather_keys(keys)
    own, half = prepare(place[1:], expert_rows, norm_gain, route_ids, route_logits, experts)
    query_rows, half = lax.optimization_barrier((query_rows, half))
    attended = attend(query_rows, gathered)
    routed_out, pieces = route_experts(
        own, half, place, attended, gate_weight, up_weight, down_weight
    )
    mixer_out = mix_heads(pieces, mixer_weight, queries.shape[2])
    return (mixer_out, routed_out)


def solution(mesh):
    in_specs = (
        P("tp", None, None, "ep"),
        P("tp", None, None, "ep"),
        P("tp", None, None, "ep"),
        P(),
        P("ep", None),
        P(),
        P("ep", None),
        P("ep", None),
        P("ep", None, "tp"),
        P("ep", None, "tp"),
        P("ep", "tp", None),
    )
    out_specs = (P(None, ("ep", "tp"), None), P("tp", "ep"))

    return jax.shard_map(body, mesh=mesh, in_specs=in_specs, out_specs=out_specs, check_vma=False)
```
